32 devices in a mesh: sp: 8 (over z, y), tp: 4 (over x, core).
Axes of the slice: x: 2, y: 2, z: 4, core: 2. Of those that a mesh axis runs over, the one named last changes fastest.
Arguments:
- queries: bfloat16 [1024, 1024], P('sp', 'tp'), may hold values from -600 to 600, as said below
- keys: bfloat16 [1024, 256], P('sp', 'tp'), may hold values from -6 to 6
- values: bfloat16 [1024, 256], P('sp', 'tp'), may hold values from -18 to 18
- forget_prefix_log: float32 [1024, 16], P('sp', 'tp'), as said below
- residual: bfloat16 [1024, 2048], P(('sp', 'tp')), may hold values from -6 to 6
- out_weight: bfloat16 [1024, 2048], replicated, may hold values from -0.1875 to 0.1875
- norm_gain: float32 [2048], replicated, may hold values from 0.1 to 1.9
- routes: int32 [1024, 2], P(('sp', 'tp')), may hold values from 0 to 7, all different within a row; in each aligned block of 32 rows (0 to 31, 32 to 63, ...) at most 16 rows name the same one
- route_weight: float32 [1024, 2], P(('sp', 'tp')), may hold values from 0.1 to 1
- w_gate: bfloat16 [8, 2048, 1024], P('sp', None, 'tp'), may hold values from -0.125 to 0.125
- w_up: bfloat16 [8, 2048, 1024], P('sp', None, 'tp'), may hold values from -0.125 to 0.125
- w_down: bfloat16 [8, 1024, 2048], P('sp', 'tp'), may hold values from -0.1875 to 0.1875
Outputs:
- layer_out: bfloat16 [1024, 2048], P(('sp', 'tp'))
The draws below stay inside these ranges and needn't reach their ends.
Inputs may be any that keep to these rules, and one draw needn't show every extreme that they name: `queries`: queries are of order one except for a few positions. `forget_prefix_log`: never rising along positions. `routes`: within the rows of one device (32 positions in order), no expert is named by more than 16 rows, a bound that some block reaches; the experts of one row differ.
All inputs are finite; a program needn't handle non-finite values.
Results may differ from the reference program's by a relative error of at most 0.013.
Values may be sent and summed in bfloat16 or wider, within the bound.
A program may use at most 64 MiB of HBM per device.

```python
import math
import jax
import jax.numpy as jnp
import numpy as np
from jax import lax

D = 2048
HEADS = 16
KV_HEADS = 4
HEAD_DIM = 64
D_EXPERT = 1024
TOP = 2
TOK_DEV = 128
LENGTH_POSITIONS = 1024
EXPERTS = 8
CAP = 16
N_SP = 8
N_TP = 4


def drawn_pair(key):
    base = jax.random.fold_in(key, 101)
    key_query, key_keys = jax.random.split(base, 2)
    query_raw = jnp.clip(jax.random.normal(key_query, (LENGTH_POSITIONS, HEADS * HEAD_DIM), jnp.float32), -6.0, 6.0)
    keys_raw = jnp.clip(jax.random.normal(key_keys, (LENGTH_POSITIONS, KV_HEADS * HEAD_DIM), jnp.float32), -6.0, 6.0)
    return (query_raw, keys_raw)


def draw_queries(key, part):
    return drawn_pair(key)[0].astype(jnp.bfloat16)


def draw_keys(key, part):
    return drawn_pair(key)[1].astype(jnp.bfloat16)


def draw_forget_prefix_log(key, part):
    base = jax.random.fold_in(key, 202)
    attended_entries_list = jax.random.split(base, 7)
    slow_share = 0.5
    lagging_attention_heads = jax.random.uniform(attended_entries_list[0], (HEADS,)) < slow_share
    slow_total = jax.random.uniform(attended_entries_list[1], (HEADS,), jnp.float32, 0.4, 1.0)
    fast_reach = jnp.exp(jax.random.uniform(attended_entries_list[2], (HEADS,), jnp.float32, math.log(30.0), math.log(100.0)))
    rate = jnp.where(lagging_attention_heads, slow_total / LENGTH_POSITIONS, 1.0 / fast_reach)
    block_factor = jnp.exp(jax.random.uniform(attended_entries_list[3], (LENGTH_POSITIONS // TOK_DEV, HEADS), jnp.float32, math.log(0.5), math.log(2.0)))
    block_factor = jnp.repeat(block_factor, TOK_DEV, axis=0)
    position_factor = jnp.exp(0.5 * jax.random.normal(attended_entries_list[4], (LENGTH_POSITIONS, HEADS), jnp.float32))
    log_forget_factor = -rate[None, :] * block_factor * position_factor
    position_batches = jax.random.randint(attended_entries_list[5], (2,), 0, LENGTH_POSITIONS)
    position_tallies = jax.random.uniform(attended_entries_list[6], (2, HEADS), jnp.float32, 0.22, 0.51)
    log_forget_factor = log_forget_factor.at[position_batches].add(-position_tallies)
    return jnp.cumsum(log_forget_factor, axis=0)


def steps_of(stream_key, dims, cuts, smallest, high):
    factor_of, own = 1.0, jax.random.fold_in(stream_key, 6)
    for dim, blocks in cuts:
        steps = jnp.exp(jax.random.uniform(jax.random.fold_in(own, dim), (blocks,), jnp.float32, smallest / len(cuts), high / len(cuts)))
        factor_of = factor_of * jnp.repeat(steps, dims[dim] // blocks).reshape([-1 if axis == dim else 1 for axis in range(len(dims))])
    return factor_of


def shared_out(key, own, number, rows, count, top, reach, skew):
    order = jax.random.permutation(key, count)
    crowded, common = shares(count, rows * top, reach, skew, True), shares(count, rows * top, reach, skew, False)
    places = jnp.arange(count)

    def named(lengths, rotation):
        used = int((lengths > 0).sum())
        fixed = max(1, used // 4)
        passed = fixed + (places - fixed + rotation * (used - fixed)) % max(1, count - fixed)
        return jnp.zeros((count,), jnp.int32).at[order[jnp.where(places < fixed, places, passed)]].set(jnp.asarray(lengths, jnp.int32))

    lengths = jnp.where(number % 4 == 0, named(crowded, number // 4), named(common, number - number // 4 - 1))
    mixed = jax.random.permutation(jax.random.fold_in(own, 3), count)
    giver, receiver = mixed[0:count // 2 * 2:2], mixed[1:count // 2 * 2:2]
    margin = jnp.minimum(lengths[giver] - 1, reach - lengths[receiver]) // 2
    margin = jnp.where((giver == order[0]) | (receiver == order[0]) | (lengths[receiver] == 0), 0, jnp.maximum(margin, 0))
    passed = jax.random.randint(jax.random.fold_in(own, 4), (count // 2,), 0, 1 << 20) % (margin + 1)
    lengths = lengths.at[giver].add(-passed).at[receiver].add(passed)
    members = jnp.searchsorted(jnp.cumsum(lengths), jnp.arange(rows * top), side="right").astype(jnp.int32)
    grid = members.reshape(top, rows).T
    grid = grid[jax.random.permutation(jax.random.fold_in(own, 1), rows)]
    rotation = jax.random.randint(jax.random.fold_in(own, 2), (rows, 1), 0, top)
    return jnp.take_along_axis(grid, (jnp.arange(top)[None, :] + rotation) % top, axis=1)


def shares(amount, total, bound, skew, full):
    loads = [(1 << 20) // math.isqrt(grade ** skew) + 1 for grade in range(1, amount + 1)]
    largest = bound if full else min(bound, max(-(-total // amount), total * loads[0] // sum(loads)))
    least = 1 if total - largest >= amount - 1 else 0
    given, rest = [largest] + [least] * (amount - 1), total - largest - least * (amount - 1)
    while rest > 0:
        movable = [i for i in range(1, amount) if given[i] < largest] or [i for i in range(1, amount) if given[i] < bound]
        whole, budget = sum([loads[i] for i in movable]), rest
        for i in movable:
            more = min(bound - given[i], max(1, budget * loads[i] // whole), rest)
            given[i] = given[i] + more
            rest = rest - more
    return np.array(given)


def scatter_about(rng, extent, deviation, bound, cuts=(), held_as=jnp.bfloat16):
    array = jax.random.normal(rng, extent, jnp.float32) * deviation
    if len(cuts) > 0:
        array = steps_of(rng, extent, cuts, -0.22, 0.18) * array
    return jnp.clip(array, min=-bound, max=bound).astype(held_as)


def setup_inputs(seed: int = 0) -> dict:
    streams_of = jax.random.split(jax.random.key(seed), 13)
    queries = draw_queries(jax.random.fold_in(streams_of[12], 71), 0)
    keys = draw_keys(jax.random.fold_in(streams_of[12], 71), 0)
    values = scatter_about(streams_of[2], (LENGTH_POSITIONS, KV_HEADS * HEAD_DIM), 3.0, 18.0, ((0, 8), (1, 4)))
    forget_prefix_log = draw_forget_prefix_log(jax.random.fold_in(streams_of[12], 71), 0)
    residual = scatter_about(streams_of[4], (LENGTH_POSITIONS, D), 1.0, 6.0, ((0, 32),))
    out_weight = scatter_about(streams_of[5], (HEADS * HEAD_DIM, D), (HEADS * HEAD_DIM) ** -0.5, 0.1875)
    norm_gain = jnp.clip(1.0 + 0.18 * jax.random.normal(streams_of[6], (D,), jnp.float32), 0.1, 1.9)
    routes_keys = jax.random.split(jax.random.fold_in(streams_of[7], 1), LENGTH_POSITIONS // (TOK_DEV // N_TP))
    routes_turns = jax.random.permutation(jax.random.fold_in(streams_of[7], 3), LENGTH_POSITIONS // (TOK_DEV // N_TP))
    routes = jax.vmap(lambda own, number: shared_out(jax.random.fold_in(streams_of[7], 2), own, number, TOK_DEV // N_TP, EXPERTS, TOP, CAP, 1))(routes_keys, routes_turns).reshape((LENGTH_POSITIONS, TOP))
    route_weight = jnp.clip(0.1 + 0.9 * jax.random.uniform(streams_of[8], (LENGTH_POSITIONS, TOP), jnp.float32) ** steps_of(streams_of[8], (LENGTH_POSITIONS, TOP), ((0, 32),), -0.2, 0.2), 0.1, 1.0)
    w_gate = scatter_about(streams_of[9], (EXPERTS, D, D_EXPERT), D ** -0.5, 0.125, ((0, 8), (2, 4)))
    w_up = scatter_about(streams_of[10], (EXPERTS, D, D_EXPERT), D ** -0.5, 0.125, ((0, 8), (2, 4)))
    w_down = scatter_about(streams_of[11], (EXPERTS, D_EXPERT, D), D_EXPERT ** -0.5, 0.1875, ((0, 8), (1, 4)))
    return dict(queries=queries, keys=keys, values=values, forget_prefix_log=forget_prefix_log, residual=residual, out_weight=out_weight, norm_gain=norm_gain, routes=routes, route_weight=route_weight, w_gate=w_gate, w_up=w_up, w_down=w_down)


def reference(queries, keys, values, forget_prefix_log, residual, out_weight, norm_gain, routes, route_weight, w_gate, w_up, w_down):
    group_size = HEADS // KV_HEADS
    block_rows = math.gcd(LENGTH_POSITIONS, 128)
    score_scale = HEAD_DIM ** (-0.5)
    query_all = queries.astype(jnp.float32).reshape(LENGTH_POSITIONS, KV_HEADS, group_size, HEAD_DIM)
    key_all = keys.astype(jnp.float32).reshape(LENGTH_POSITIONS, KV_HEADS, HEAD_DIM)
    value_all = values.astype(jnp.float32).reshape(LENGTH_POSITIONS, KV_HEADS, HEAD_DIM)
    gates_heads = forget_prefix_log.reshape(LENGTH_POSITIONS, KV_HEADS, group_size).transpose(1, 2, 0)
    key_pos = jnp.arange(LENGTH_POSITIONS, dtype=jnp.int32)

    def attend_block(block_index):
        first_row = (block_index * block_rows).astype(jnp.int32)
        query_block = lax.dynamic_slice_in_dim(query_all, first_row, block_rows, 0)
        gate_block = lax.dynamic_slice_in_dim(gates_heads, first_row, block_rows, 2)
        scores = jnp.einsum('tkgd,skd->kgts', query_block, key_all) * score_scale
        scores = scores + gate_block[..., None] - gates_heads[:, :, None, :]
        causal = (first_row + jnp.arange(block_rows, dtype=jnp.int32))[:, None] >= key_pos[None, :]
        scores = jnp.where(causal, scores, -1e+30)
        row_peak = lax.optimization_barrier(jnp.max(scores, axis=-1, keepdims=True))
        weights = jnp.where(causal, jnp.exp(scores - row_peak), 0.0)
        row_total = lax.optimization_barrier(jnp.sum(weights, axis=-1))
        rounded = lax.optimization_barrier(weights.astype(jnp.bfloat16)).astype(jnp.float32)
        weighted = jnp.einsum('kgts,skd->tkgd', rounded, value_all)
        result = weighted / row_total.transpose(2, 0, 1)[..., None]
        return result.astype(jnp.bfloat16).reshape(block_rows, HEADS * HEAD_DIM)
    attended = lax.map(attend_block, jnp.arange(LENGTH_POSITIONS // block_rows, dtype=jnp.int32))
    attended = attended.reshape(LENGTH_POSITIONS, HEADS * HEAD_DIM)
    stream = residual.astype(jnp.float32) + jnp.dot(attended, out_weight, preferred_element_type=jnp.float32)
    mean_square = lax.optimization_barrier(jnp.mean(stream * stream, axis=-1, keepdims=True))
    normed = (stream * lax.rsqrt(mean_square + 1e-06) * norm_gain.astype(jnp.float32)).astype(jnp.bfloat16)
    assigned = LENGTH_POSITIONS * TOP
    flat_expert = routes.reshape(assigned)
    flat_weight = route_weight.reshape(assigned)
    order = jnp.argsort(flat_expert, stable=True).astype(jnp.int32)
    counts = lax.optimization_barrier(jnp.sum((flat_expert[:, None] == jnp.arange(EXPERTS, dtype=jnp.int32)[None, :]).astype(jnp.int32), axis=0))
    starts = jnp.cumsum(counts) - counts
    most_rows = N_SP * N_TP * CAP
    quarter = D_EXPERT // N_TP

    def one_expert(running_total, expert):
        offsets = jnp.arange(most_rows, dtype=jnp.int32)
        valid = offsets < counts[expert]
        chosen = order[jnp.minimum(starts[expert] + offsets, assigned - 1)]
        position = chosen // TOP
        picked = normed[position]
        gate_act = jnp.dot(picked, w_gate[expert], preferred_element_type=jnp.float32)
        up_act = jnp.dot(picked, w_up[expert], preferred_element_type=jnp.float32)
        activated = (jax.nn.silu(gate_act) * up_act).astype(jnp.bfloat16)
        summed = jnp.zeros((most_rows, D), jnp.float32)
        for quarter_index in range(N_TP):
            partial_out = jnp.dot(activated[:, quarter_index * quarter:(quarter_index + 1) * quarter], w_down[expert][quarter_index * quarter:(quarter_index + 1) * quarter], preferred_element_type=jnp.float32).astype(jnp.bfloat16)
            summed = summed + lax.optimization_barrier(partial_out).astype(jnp.float32)
        expert_out = lax.optimization_barrier(summed.astype(jnp.bfloat16)).astype(jnp.float32)
        scaled = jnp.where(valid, flat_weight[chosen], 0.0)
        return (running_total.at[position].add(scaled[:, None] * expert_out), None)
    mixture, unused = lax.scan(one_expert, jnp.zeros((LENGTH_POSITIONS, D), jnp.float32), jnp.arange(EXPERTS, dtype=jnp.int32))
    return (stream + mixture).astype(jnp.bfloat16)
```

```python
import functools

import jax
import jax.numpy as jnp
from jax import lax
from jax.experimental import pallas as pl
from jax.experimental.pallas import tpu as pltpu
from jax.sharding import PartitionSpec as P

HEAD_DIM = 64
MESH = pl.DeviceIdType.MESH
F32 = jnp.float32
BF16 = jnp.bfloat16


def each(first, last, body):
    def step(i, carry):
        body(i)
        return carry

    lax.fori_loop(first, last, step, 0)


def layer_kernel(
    n_sp,
    n_tp,
    q_ref,
    kv_ref,
    gate_ref,
    residual_ref,
    gain_ref,
    routes_ref,
    routes_t_ref,
    route_weight_ref,
    ow_hbm,
    wg_hbm,
    wu_hbm,
    wd_hbm,
    out_ref,
    kv_all,
    gate_all,
    attended,
    swapped,
    stream,
    ow,
    wg,
    wu,
    wd,
    outgoing,
    pool,
    core_part,
    x_stage,
    x_part,
    back_stage,
    back,
    kept,
    kept_own,
    local_sem,
    kv_sem,
    gate_sem,
    swap_sem,
    disp_sem,
    xf_sem,
    cf_sem,
    cf2_sem,
    core_sem,
    x_sem,
    ret_sem,
):
    s = lax.axis_index("sp")
    t = lax.axis_index("tp")
    t_core = t + 1 - 2 * lax.rem(t, 2)
    t_x = t + 2 - 4 * lax.rem(lax.div(t, 2), 2)
    tok = q_ref.shape[0]
    heads = gate_ref.shape[0]
    tok_row, width = residual_ref.shape
    capp = outgoing.shape[1]
    slots = n_sp * capp
    head_cols = heads * HEAD_DIM

    def remote(src, dst, sems, index, to):
        return pltpu.make_async_remote_copy(
            src_ref=src,
            dst_ref=dst,
            send_sem=sems.at[0, index],
            recv_sem=sems.at[1, index],
            device_id=to,
            device_id_type=MESH,
        )

    loads = [
        pltpu.make_async_copy(a, b, local_sem.at[i])
        for i, (a, b) in enumerate(
            [(ow_hbm, ow), (wg_hbm.at[0], wg), (wu_hbm.at[0], wu), (wd_hbm.at[0], wd)]
        )
    ]
    for load in loads:
        load.start()

    barrier = pltpu.get_barrier_semaphore()

    def greet_sp(d):
        pl.semaphore_signal(
            barrier, inc=1, device_id=(lax.rem(s + d, n_sp), t), device_id_type=MESH
        )

    def greet_tp(k):
        pl.semaphore_signal(
            barrier, inc=1, device_id=(s, lax.rem(t + k, n_tp)), device_id_type=MESH
        )

    each(1, n_sp, greet_sp)
    each(1, n_tp, greet_tp)
    pl.semaphore_wait(barrier, n_sp - 1 + n_tp - 1)

    def kv_copy(d):
        return remote(kv_ref, kv_all.at[d], kv_sem, d, (lax.rem(s + d, n_sp), t))

    def gate_copy(d):
        return remote(gate_ref, gate_all.at[d], gate_sem, d, (lax.rem(s + d, n_sp), t))

    def send_kv(d):
        kv_copy(d).start()
        gate_copy(d).start()

    each(1, n_sp - s, send_kv)

    rows_i = lax.broadcasted_iota(jnp.int32, (tok_row, tok_row), 0)
    cols_i = lax.broadcasted_iota(jnp.int32, (tok_row, tok_row), 1)
    top = routes_ref.shape[1]
    col = [routes_ref[:, k : k + 1] for k in range(top)]
    row = [routes_t_ref[k : k + 1, :] for k in range(top)]
    slot_row, slot_col = [], []
    for k in range(top):
        rank_row = jnp.zeros((1, tok_row), F32)
        rank_col = jnp.zeros((tok_row, 1), F32)
        for other in range(top):
            same = jnp.logical_and(col[other] == row[k], rows_i < cols_i)
            rank_row = rank_row + jnp.sum(jnp.where(same, 1.0, 0.0), axis=0, keepdims=True)
            same = jnp.logical_and(row[other] == col[k], cols_i < rows_i)
            rank_col = rank_col + jnp.sum(jnp.where(same, 1.0, 0.0), axis=1, keepdims=True)
        slot_row.append((lax.rem(row[k] - s + n_sp, n_sp) * capp).astype(F32) + rank_row)
        slot_col.append((lax.rem(col[k] - s + n_sp, n_sp) * capp).astype(F32) + rank_col)
    slot_of_row = lax.broadcasted_iota(jnp.int32, (slots, tok_row), 0).astype(F32)
    slot_of_col = lax.broadcasted_iota(jnp.int32, (tok_row, slots), 1).astype(F32)
    spread = jnp.zeros((slots, tok_row), F32)
    for k in range(top):
        spread = spread + jnp.where(slot_of_row == slot_row[k], 1.0, 0.0)
    spread = spread.astype(BF16)

    query = q_ref[...] * jnp.asarray(HEAD_DIM**-0.5, BF16)
    stacked = jnp.concatenate(
        [query[:, h * HEAD_DIM : (h + 1) * HEAD_DIM] for h in range(heads)], axis=0
    )

    def scores_of(kv, gate):
        raw = lax.dot_general(
            stacked,
            kv[:, :HEAD_DIM],
            (((1,), (1,)), ((), ())),
            preferred_element_type=F32,
        )
        return raw.reshape(heads, tok, tok) - gate[:, None, :]

    def weigh(weights, kv):
        return jnp.dot(
            weights.astype(BF16).reshape(heads * tok, tok),
            kv[:, HEAD_DIM:],
            preferred_element_type=F32,
        ).reshape(heads, tok, HEAD_DIM)

    kv_own = kv_ref[...]
    scores = scores_of(kv_own, gate_ref[...])
    causal = lax.broadcasted_iota(jnp.int32, (heads, tok, tok), 1) >= lax.broadcasted_iota(
        jnp.int32, (heads, tok, tok), 2
    )
    scores = jnp.where(causal, scores, -1e30)
    peak = jnp.max(scores, axis=-1, keepdims=True)
    weights = jnp.exp(scores - peak)
    total = jnp.sum(weights, axis=-1, keepdims=True)
    weighted = weigh(weights, kv_own)

    def absorb(d, state):
        peak, total, weighted = state
        kv_copy(d).wait_recv()
        gate_copy(d).wait_recv()
        kv = kv_all[d]
        scores = scores_of(kv, gate_all[d])
        new_peak = jnp.maximum(peak, jnp.max(scores, axis=-1, keepdims=True))
        weights = jnp.exp(scores - new_peak)
        shrink = jnp.exp(peak - new_peak)
        total = total * shrink + jnp.sum(weights, axis=-1, keepdims=True)
        weighted = weighted * shrink + weigh(weights, kv)
        return new_peak, total, weighted

    peak, total, weighted = lax.fori_loop(1, s + 1, absorb, (peak, total, weighted))
    result = (weighted / total).astype(BF16)
    for h in range(heads):
        attended[:, h * HEAD_DIM : (h + 1) * HEAD_DIM] = result[h]

    def rows_of(p):
        return pl.ds(pl.multiple_of(p * tok_row, tok_row), tok_row)

    def swap_copy(k):
        p = lax.rem(t + k, n_tp)
        return remote(attended.at[rows_of(p)], swapped.at[k], swap_sem, k, (s, p))

    for k in range(1, n_tp):
        swap_copy(k).start()
    loads[0].wait()

    def weight_rows(p):
        return ow[pl.ds(pl.multiple_of(p * head_cols, head_cols), head_cols), :]

    total_stream = residual_ref[...].astype(F32) + jnp.dot(
        attended[rows_of(t), :], weight_rows(t), preferred_element_type=F32
    )
    for k in range(1, n_tp):
        swap_copy(k).wait_recv()
        total_stream = total_stream + jnp.dot(
            swapped[k], weight_rows(lax.rem(t - k + n_tp, n_tp)), preferred_element_type=F32
        )
    stream[...] = total_stream
    mean_square = jnp.mean(total_stream * total_stream, axis=-1, keepdims=True)
    normed = (total_stream * lax.rsqrt(mean_square + 1e-06) * gain_ref[...]).astype(BF16)

    dispatched = jnp.dot(spread, normed, preferred_element_type=F32).astype(BF16)
    outgoing[...] = dispatched.reshape(n_sp, capp, width)
    pool[0, 0] = dispatched[:capp]

    def disp_copy(d):
        return remote(
            outgoing.at[d], pool.at[d, 0], disp_sem, d, (lax.rem(s + d, n_sp), t)
        )

    each(1, n_sp, lambda d: disp_copy(d).start())

    def xf_copy(d):
        return remote(pool.at[d, 0], pool.at[d, 1], xf_sem, d, (s, t_x))

    def cf_copy(d):
        return remote(pool.at[d, 0], pool.at[d, 2], cf_sem, d, (s, t_core))

    def cf2_copy(d):
        return remote(pool.at[d, 1], pool.at[d, 3], cf2_sem, d, (s, t_core))

    def core_copy(d):
        return remote(pool.at[d, pl.ds(2, 2)], core_part.at[d], core_sem, d, (s, t_core))

    def x_copy(d):
        return remote(x_stage.at[d], x_part.at[d], x_sem, d, (s, t_x))

    def ret_copy(d):
        return remote(
            back_stage.at[d], back.at[d], ret_sem, d, (lax.rem(s - d + n_sp, n_sp), t)
        )

    for load in loads[1:]:
        load.wait()

    def stage(i, lag, body):
        d = i - lag

        @pl.when(jnp.logical_and(d >= 0, d < n_sp))
        def _():
            body(d)

    def arrive(d):
        @pl.when(d > 0)
        def _():
            disp_copy(d).wait_recv()

        xf_copy(d).start()
        cf_copy(d).start()

    def relay(d):
        xf_copy(d).wait_recv()
        cf2_copy(d).start()

    def compute(d):
        cf_copy(d).wait_recv()
        cf2_copy(d).wait_recv()
        picked = pool[d].reshape(4 * capp, width)
        gate_act = jnp.dot(picked, wg[...], preferred_element_type=F32)
        up_act = jnp.dot(picked, wu[...], preferred_element_type=F32)
        hidden = (gate_act / (1.0 + jnp.exp(-gate_act)) * up_act).astype(BF16)
        part = jnp.dot(hidden, wd[...], preferred_element_type=F32)
        pool[d, pl.ds(2, 2)] = part[2 * capp :].astype(BF16).reshape(2, capp, width)
        kept[lax.rem(d, 2)] = part[: 2 * capp]
        core_copy(d).start()

    def over_cores(d):
        core_copy(d).wait_recv()
        both = kept[lax.rem(d, 2)] + core_part[d].reshape(2 * capp, width).astype(F32)
        x_stage[d] = both[capp:].astype(BF16)
        kept_own[lax.rem(d, 2)] = both[:capp]
        x_copy(d).start()

    def over_x(d):
        x_copy(d).wait_recv()
        done = (kept_own[lax.rem(d, 2)] + x_part[d].astype(F32)).astype(BF16)

        @pl.when(d == 0)
        def _():
            back[0] = done

        @pl.when(d > 0)
        def _():
            back_stage[d] = done
            ret_copy(d).start()

    def pipeline(i):
        stage(i, 0, arrive)
        stage(i, 1, relay)
        stage(i, 4, over_x)
        stage(i, 3, over_cores)
        stage(i, 2, compute)

    each(0, n_sp + 4, pipeline)

    combine = jnp.zeros((tok_row, slots), F32)
    for k in range(top):
        combine = combine + jnp.where(
            slot_of_col == slot_col[k], route_weight_ref[:, k : k + 1], 0.0
        )
    high = combine.astype(BF16)
    low = (combine - high.astype(F32)).astype(BF16)
    each(1, n_sp, lambda d: ret_copy(d).wait_recv())
    returned = back[...].reshape(slots, width)
    mixture = jnp.dot(high, returned, preferred_element_type=F32) + jnp.dot(
        low, returned, preferred_element_type=F32
    )
    out_ref[...] = (stream[...] + mixture).astype(out_ref.dtype)

    def sent_kv(d):
        kv_copy(d).wait_send()
        gate_copy(d).wait_send()

    each(1, n_sp - s, sent_kv)
    for k in range(1, n_tp):
        swap_copy(k).wait_send()

    def sent(d):
        @pl.when(d > 0)
        def _():
            disp_copy(d).wait_send()
            ret_copy(d).wait_send()

        for copy in (xf_copy, cf_copy, cf2_copy, core_copy, x_copy):
            copy(d).wait_send()

    each(0, n_sp, sent)


def shards(
    n_sp,
    n_tp,
    queries,
    keys,
    values,
    forget_prefix_log,
    residual,
    out_weight,
    norm_gain,
    routes,
    route_weight,
    w_gate,
    w_up,
    w_down,
):
    tok = queries.shape[0]
    heads = forget_prefix_log.shape[1]
    assert keys.shape[1] == HEAD_DIM and n_tp == 4
    tok_row, width = residual.shape
    capacity = max(2, 2 * tok_row * routes.shape[1] // n_sp)
    capp = -(-capacity // 16) * 16
    quarter = w_gate.shape[2]
    kv = jnp.concatenate([keys, values], axis=1)
    vmem = pl.BlockSpec(memory_space=pltpu.VMEM)
    hbm = pl.BlockSpec(memory_space=pl.ANY)
    sems = lambda n: pltpu.SemaphoreType.DMA((2, n))
    block = (n_sp, capp, width)
    return pl.pallas_call(
        functools.partial(layer_kernel, n_sp, n_tp),
        out_shape=jax.ShapeDtypeStruct((tok_row, width), BF16),
        in_specs=[vmem] * 8 + [hbm] * 4,
        out_specs=vmem,
        scratch_shapes=[
            pltpu.VMEM((n_sp, tok, 2 * HEAD_DIM), BF16),
            pltpu.VMEM((n_sp, heads, tok), F32),
            pltpu.VMEM((tok, heads * HEAD_DIM), BF16),
            pltpu.VMEM((n_tp, tok_row, heads * HEAD_DIM), BF16),
            pltpu.VMEM((tok_row, width), F32),
            pltpu.VMEM(out_weight.shape, BF16),
            pltpu.VMEM((width, quarter), BF16),
            pltpu.VMEM((width, quarter), BF16),
            pltpu.VMEM((quarter, width), BF16),
            pltpu.VMEM(block, BF16),
            pltpu.VMEM((n_sp, 4, capp, width), BF16),
            pltpu.VMEM((n_sp, 2, capp, width), BF16),
            pltpu.VMEM(block, BF16),
            pltpu.VMEM(block, BF16),
            pltpu.VMEM(block, BF16),
            pltpu.VMEM(block, BF16),
            pltpu.VMEM((2, 2 * capp, width), F32),
            pltpu.VMEM((2, capp, width), F32),
            pltpu.SemaphoreType.DMA((4,)),
            sems(n_sp),
            sems(n_sp),
            sems(n_tp),
            sems(n_sp),
            sems(n_sp),
            sems(n_sp),
            sems(n_sp),
            sems(n_sp),
            sems(n_sp),
            sems(n_sp),
        ],
        compiler_params=pltpu.CompilerParams(
            collective_id=0, has_side_effects=True, vmem_limit_bytes=66_000_000
        ),
    )(
        queries,
        kv,
        forget_prefix_log.T,
        residual,
        norm_gain.reshape(1, width),
        routes,
        routes.T,
        route_weight,
        out_weight,
        w_gate,
        w_up,
        w_down,
    )


def solution(mesh):
    return jax.shard_map(
        functools.partial(shards, mesh.shape["sp"], mesh.shape["tp"]),
        mesh=mesh,
        in_specs=(
            P("sp", "tp"),
            P("sp", "tp"),
            P("sp", "tp"),
            P("sp", "tp"),
            P(("sp", "tp"), None),
            P(),
            P(),
            P(("sp", "tp"), None),
            P(("sp", "tp"), None),
            P("sp", None, "tp"),
            P("sp", None, "tp"),
            P("sp", "tp", None),
        ),
        out_specs=P(("sp", "tp"), None),
        check_vma=False,
    )
```

```python
import functools

import jax
import jax.numpy as jnp
from jax import lax
from jax.experimental import pallas as pl
from jax.experimental.pallas import tpu as pltpu
from jax.sharding import PartitionSpec as P

HEAD_DIM = 64
MESH = pl.DeviceIdType.MESH
F32 = jnp.float32
BF16 = jnp.bfloat16


def each(first, last, body):
    def step(i, carry):
        body(i)
        return carry

    lax.fori_loop(first, last, step, 0)


def layer_kernel(
    n_sp,
    n_tp,
    q_ref,
    key_ref,
    value_ref,
    gate_ref,
    residual_ref,
    gain_ref,
    routes_ref,
    route_weight_ref,
    ow_hbm,
    wg_hbm,
    wu_hbm,
    wd_hbm,
    out_ref,
    kv_all,
    gate_all,
    attended,
    swapped,
    stream,
    ow,
    wg,
    wu,
    wd,
    outgoing,
    pool,
    core_part,
    x_part,
    back,
    local_sem,
    key_sem,
    value_sem,
    gate_sem,
    swap_sem,
    disp_sem,
    xf_sem,
    cf_sem,
    cf2_sem,
    core_sem,
    x_sem,
    ret_sem,
):
    s = lax.axis_index("sp")
    t = lax.axis_index("tp")
    t_core = t + 1 - 2 * lax.rem(t, 2)
    t_x = t + 2 - 4 * lax.rem(lax.div(t, 2), 2)
    tok = q_ref.shape[0]
    heads = gate_ref.shape[0]
    tok_row, width = residual_ref.shape
    capp = outgoing.shape[1]
    slots = n_sp * capp
    head_cols = heads * HEAD_DIM

    def partner(a, b):
        both, bit = 0, 1
        while bit < n_sp:
            both = both + bit * (lax.rem(lax.div(a, bit), 2) * lax.rem(lax.div(b, bit), 2))
            bit *= 2
        return a + b - 2 * both

    def remote(src, dst, sems, index, to):
        return pltpu.make_async_remote_copy(
            src_ref=src,
            dst_ref=dst,
            send_sem=sems.at[0, index],
            recv_sem=sems.at[1, index],
            device_id=to,
            device_id_type=MESH,
        )

    loads = [
        pltpu.make_async_copy(a, b, local_sem.at[i])
        for i, (a, b) in enumerate(
            [(ow_hbm, ow), (wg_hbm.at[0], wg), (wu_hbm.at[0], wu), (wd_hbm.at[0], wd)]
        )
    ]
    for load in loads:
        load.start()

    barrier = pltpu.get_barrier_semaphore()

    def greet_sp(d):
        pl.semaphore_signal(
            barrier, inc=1, device_id=(lax.rem(s + d, n_sp), t), device_id_type=MESH
        )

    def greet_tp(k):
        pl.semaphore_signal(
            barrier, inc=1, device_id=(s, lax.rem(t + k, n_tp)), device_id_type=MESH
        )

    each(1, n_sp, greet_sp)
    each(1, n_tp, greet_tp)
    pl.semaphore_wait(barrier, n_sp - 1 + n_tp - 1)

    def kv_copies(d):
        to = (lax.rem(s + d, n_sp), t)
        return (
            remote(key_ref, kv_all.at[d, pl.ds(0, HEAD_DIM)], key_sem, d, to),
            remote(value_ref, kv_all.at[d, pl.ds(HEAD_DIM, HEAD_DIM)], value_sem, d, to),
            remote(gate_ref, gate_all.at[d], gate_sem, d, to),
        )

    def send_kv(d):
        for copy in kv_copies(d):
            copy.start()

    each(1, n_sp - s, send_kv)

    rows_i = lax.broadcasted_iota(jnp.int32, (tok_row, tok_row), 0)
    cols_i = lax.broadcasted_iota(jnp.int32, (tok_row, tok_row), 1)
    top = routes_ref.shape[0]
    row = [routes_ref[k : k + 1, :] for k in range(top)]

    def upright(line):
        return jnp.sum(jnp.where(rows_i == cols_i, line, 0.0), axis=1, keepdims=True)

    col = [upright(row[k].astype(F32)) for k in range(top)]
    slot_row, slot_col = [], []
    for k in range(top):
        rank_row = jnp.zeros((1, tok_row), F32)
        for other in range(top):
            same = jnp.logical_and(col[other] == row[k].astype(F32), rows_i < cols_i)
            rank_row = rank_row + jnp.sum(jnp.where(same, 1.0, 0.0), axis=0, keepdims=True)
        slot_row.append((partner(row[k], s) * capp).astype(F32) + rank_row)
        slot_col.append(upright(slot_row[k]))
    slot_of_row = lax.broadcasted_iota(jnp.int32, (slots, tok_row), 0).astype(F32)
    slot_of_col = lax.broadcasted_iota(jnp.int32, (tok_row, slots), 1).astype(F32)
    spread = jnp.zeros((slots, tok_row), F32)
    for k in range(top):
        spread = spread + jnp.where(slot_of_row == slot_row[k], 1.0, 0.0)
    spread = spread.astype(BF16)

    query = q_ref[...] * jnp.asarray(HEAD_DIM**-0.5, BF16)
    stacked = jnp.concatenate(
        [query[:, h * HEAD_DIM : (h + 1) * HEAD_DIM] for h in range(heads)], axis=0
    )

    def scores_of(key, gate):
        raw = jnp.dot(stacked, key, preferred_element_type=F32)
        return raw.reshape(heads, tok, tok) - gate[:, None, :]

    def weigh(weights, value):
        return lax.dot_general(
            weights.astype(BF16).reshape(heads * tok, tok),
            value,
            (((1,), (1,)), ((), ())),
            preferred_element_type=F32,
        ).reshape(heads, tok, HEAD_DIM)

    scores = scores_of(key_ref[...], gate_ref[...])
    causal = lax.broadcasted_iota(jnp.int32, (heads, tok, tok), 1) >= lax.broadcasted_iota(
        jnp.int32, (heads, tok, tok), 2
    )
    scores = jnp.where(causal, scores, -1e30)
    peak = jnp.max(scores, axis=-1, keepdims=True)
    weights = jnp.exp(scores - peak)
    total = jnp.sum(weights, axis=-1, keepdims=True)
    weighted = weigh(weights, value_ref[...])

    def absorb(d, state):
        peak, total, weighted = state
        for copy in kv_copies(d):
            copy.wait_recv()
        scores = scores_of(kv_all[d, :HEAD_DIM], gate_all[d])
        new_peak = jnp.maximum(peak, jnp.max(scores, axis=-1, keepdims=True))
        weights = jnp.exp(scores - new_peak)
        shrink = jnp.exp(peak - new_peak)
        total = total * shrink + jnp.sum(weights, axis=-1, keepdims=True)
        weighted = weighted * shrink + weigh(weights, kv_all[d, HEAD_DIM:])
        return new_peak, total, weighted

    peak, total, weighted = lax.fori_loop(1, s + 1, absorb, (peak, total, weighted))
    result = (weighted / total).astype(BF16)
    for h in range(heads):
        attended[:, h * HEAD_DIM : (h + 1) * HEAD_DIM] = result[h]

    def rows_of(p):
        return pl.ds(pl.multiple_of(p * tok_row, tok_row), tok_row)

    def swap_copy(k):
        p = lax.rem(t + k, n_tp)
        return remote(attended.at[rows_of(p)], swapped.at[k], swap_sem, k, (s, p))

    for k in range(1, n_tp):
        swap_copy(k).start()
    loads[0].wait()

    def weight_rows(p):
        return ow[pl.ds(pl.multiple_of(p * head_cols, head_cols), head_cols), :]

    total_stream = residual_ref[...].astype(F32) + jnp.dot(
        attended[rows_of(t), :], weight_rows(t), preferred_element_type=F32
    )
    for k in range(1, n_tp):
        swap_copy(k).wait_recv()
        total_stream = total_stream + jnp.dot(
            swapped[k], weight_rows(lax.rem(t - k + n_tp, n_tp)), preferred_element_type=F32
        )
    stream[...] = total_stream
    mean_square = jnp.mean(total_stream * total_stream, axis=-1, keepdims=True)
    normed = (total_stream * lax.rsqrt(mean_square + 1e-06) * gain_ref[...]).astype(BF16)

    dispatched = jnp.dot(spread, normed, preferred_element_type=F32).astype(BF16)
    outgoing[...] = dispatched.reshape(n_sp, capp, width)
    pool[0, 0] = dispatched[:capp]

    def disp_copy(d):
        return remote(
            outgoing.at[d], pool.at[d, 0], disp_sem, d, (partner(s, d), t)
        )

    each(1, n_sp, lambda d: disp_copy(d).start())

    def xf_copy(d):
        return remote(pool.at[d, 0], pool.at[d, 1], xf_sem, d, (s, t_x))

    def cf_copy(d):
        return remote(pool.at[d, 0], pool.at[d, 2], cf_sem, d, (s, t_core))

    def cf2_copy(d):
        return remote(pool.at[d, 1], pool.at[d, 3], cf2_sem, d, (s, t_core))

    def core_copy(d):
        return remote(pool.at[d, pl.ds(2, 2)], core_part.at[d], core_sem, d, (s, t_core))

    def x_copy(d):
        return remote(pool.at[d, 1], x_part.at[d], x_sem, d, (s, t_x))

    def ret_copy(d):
        return remote(
            pool.at[d, 0], back.at[d], ret_sem, d, (partner(s, d), t)
        )

    for load in loads[1:]:
        load.wait()

    def stage(i, lag, body):
        d = i - lag

        @pl.when(jnp.logical_and(d >= 0, d < n_sp))
        def _():
            body(d)

    def arrive(d):
        @pl.when(d > 0)
        def _():
            disp_copy(d).wait_recv()

        xf_copy(d).start()
        cf_copy(d).start()

    def relay(d):
        xf_copy(d).wait_recv()
        cf2_copy(d).start()

    def compute(d):
        cf_copy(d).wait_recv()
        cf2_copy(d).wait_recv()
        picked = pool[d].reshape(4 * capp, width)
        gate_act = jnp.dot(picked, wg[...], preferred_element_type=F32)
        up_act = jnp.dot(picked, wu[...], preferred_element_type=F32)
        hidden = (gate_act / (1.0 + jnp.exp(-gate_act)) * up_act).astype(BF16)
        part = jnp.dot(hidden, wd[...], preferred_element_type=F32)
        for copy in (xf_copy, cf_copy, cf2_copy):
            copy(d).wait_send()
        pool[d] = part.astype(BF16).reshape(4, capp, width)
        core_copy(d).start()

    def over_cores(d):
        core_copy(d).wait_recv()
        both = pool[d, pl.ds(0, 2)].astype(F32) + core_part[d].astype(F32)
        pool[d, pl.ds(0, 2)] = both.astype(BF16)
        x_copy(d).start()

    def over_x(d):
        x_copy(d).wait_recv()
        done = (pool[d, 0].astype(F32) + x_part[d].astype(F32)).astype(BF16)

        @pl.when(d == 0)
        def _():
            back[0] = done

        @pl.when(d > 0)
        def _():
            pool[d, 0] = done
            ret_copy(d).start()

    def inward(i):
        stage(i, 0, arrive)
        stage(i, 1, relay)
        stage(i, 2, compute)

    each(0, n_sp + 2, inward)

    def outward(i):
        stage(i, 0, lambda d: over_cores(n_sp - 1 - d))
        stage(i, 2, lambda d: over_x(n_sp - 1 - d))

    each(0, n_sp + 2, outward)

    combine = jnp.zeros((tok_row, slots), F32)
    for k in range(top):
        combine = combine + jnp.where(
            slot_of_col == slot_col[k], upright(route_weight_ref[k : k + 1, :]), 0.0
        )
    high = combine.astype(BF16)
    low = (combine - high.astype(F32)).astype(BF16)
    each(1, n_sp, lambda d: ret_copy(d).wait_recv())
    returned = back[...].reshape(slots, width)
    mixture = jnp.dot(high, returned, preferred_element_type=F32) + jnp.dot(
        low, returned, preferred_element_type=F32
    )
    out_ref[...] = (stream[...] + mixture).astype(out_ref.dtype)

    def sent_kv(d):
        for copy in kv_copies(d):
            copy.wait_send()

    each(1, n_sp - s, sent_kv)
    for k in range(1, n_tp):
        swap_copy(k).wait_send()

    def sent(d):
        @pl.when(d > 0)
        def _():
            disp_copy(d).wait_send()
            ret_copy(d).wait_send()

        for copy in (core_copy, x_copy):
            copy(d).wait_send()

    each(0, n_sp, sent)


def shards(
    n_sp,
    n_tp,
    queries,
    keys,
    values,
    forget_prefix_log,
    residual,
    out_weight,
    norm_gain,
    routes,
    route_weight,
    w_gate,
    w_up,
    w_down,
):
    tok = queries.shape[0]
    heads = forget_prefix_log.shape[1]
    assert keys.shape[1] == HEAD_DIM and n_tp == 4 and n_sp & (n_sp - 1) == 0
    tok_row, width = residual.shape
    capacity = max(2, 2 * tok_row * routes.shape[1] // n_sp)
    capp = -(-capacity // 16) * 16
    quarter = w_gate.shape[2]
    vmem = pl.BlockSpec(memory_space=pltpu.VMEM)
    hbm = pl.BlockSpec(memory_space=pl.ANY)
    sems = lambda n: pltpu.SemaphoreType.DMA((2, n))
    block = (n_sp, capp, width)
    return pl.pallas_call(
        functools.partial(layer_kernel, n_sp, n_tp),
        out_shape=jax.ShapeDtypeStruct((tok_row, width), BF16),
        in_specs=[vmem] * 8 + [hbm] * 4,
        out_specs=vmem,
        scratch_shapes=[
            pltpu.VMEM((n_sp, 2 * HEAD_DIM, tok), BF16),
            pltpu.VMEM((n_sp, heads, tok), F32),
            pltpu.VMEM((tok, heads * HEAD_DIM), BF16),
            pltpu.VMEM((n_tp, tok_row, heads * HEAD_DIM), BF16),
            pltpu.VMEM((tok_row, width), F32),
            pltpu.VMEM(out_weight.shape, BF16),
            pltpu.VMEM((width, quarter), BF16),
            pltpu.VMEM((width, quarter), BF16),
            pltpu.VMEM((quarter, width), BF16),
            pltpu.VMEM(block, BF16),
            pltpu.VMEM((n_sp, 4, capp, width), BF16),
            pltpu.VMEM((n_sp, 2, capp, width), BF16),
            pltpu.VMEM(block, BF16),
            pltpu.VMEM(block, BF16),
            pltpu.SemaphoreType.DMA((4,)),
            sems(n_sp),
            sems(n_sp),
            sems(n_sp),
            sems(n_tp),
            sems(n_sp),
            sems(n_sp),
            sems(n_sp),
            sems(n_sp),
            sems(n_sp),
            sems(n_sp),
            sems(n_sp),
        ],
        compiler_params=pltpu.CompilerParams(
            collective_id=0, has_side_effects=True, vmem_limit_bytes=66_000_000
        ),
    )(
        queries,
        keys.T,
        values.T,
        forget_prefix_log.T,
        residual,
        norm_gain.reshape(1, width),
        routes.T,
        route_weight.T,
        out_weight,
        w_gate,
        w_up,
        w_down,
    )


def solution(mesh):
    return jax.shard_map(
        functools.partial(shards, mesh.shape["sp"], mesh.shape["tp"]),
        mesh=mesh,
        in_specs=(
            P("sp", "tp"),
            P("sp", "tp"),
            P("sp", "tp"),
            P("sp", "tp"),
            P(("sp", "tp"), None),
            P(),
            P(),
            P(("sp", "tp"), None),
            P(("sp", "tp"), None),
            P("sp", None, "tp"),
            P("sp", None, "tp"),
            P("sp", "tp", None),
        ),
        out_specs=P(("sp", "tp"), None),
        check_vma=False,
    )
```
